32 devices in a mesh: sp: 16 (over z, x, core), tp: 2 (over y).
Axes of the slice: x: 2, y: 2, z: 4, core: 2. Of those that a mesh axis runs over, the one named last changes fastest.
Arguments:
- out_gate: bfloat16 [4096, 512], P('sp', 'tp'), may hold values from -6 to 6
- in_gate: bfloat16 [4096, 512], P('sp', 'tp'), may hold values from -6 to 6
- conv_input: bfloat16 [4096, 512], P('sp', 'tp'), may hold values from -6 to 6
- conv_taps: float32 [3, 512], P(None, 'tp'), may hold values from -3.5 to 3.5
- out_weight: bfloat16 [512, 2048], P('tp'), may hold values from -0.25 to 0.25
- residual: bfloat16 [4096, 2048], P('sp', 'tp'), may hold values from -60 to 60
- document: int32 [4096], P('sp'), may hold values from 0 to 3, never falling along the last dimension, each value on 1 to 2048 neighbouring positions
- mix_gain: float32 [2048], P('tp'), may hold values from 0.15 to 3
- ffn_gain: float32 [2048], P('tp'), may hold values from 0.1 to 1.9
- routes: int32 [4096, 2], P('sp'), may hold values from 0 to 15, all different within a row; in each aligned block of 256 rows (0 to 255, 256 to 511, ...) at most 64 rows name the same one
- route_weight: float32 [4096, 2], P('sp'), may hold values from 0.1 to 1
- expert_gate: bfloat16 [16, 2048, 4096], P('sp', None, 'tp'), may hold values from -0.375 to 0.375
- expert_up: bfloat16 [16, 2048, 4096], P('sp', None, 'tp'), may hold values from -0.375 to 0.375
- expert_down: bfloat16 [16, 4096, 2048], P('sp', None, 'tp'), may hold values from -0.09375 to 0.09375
Outputs:
- result: bfloat16 [4096, 2048], P('sp', 'tp')
The draws below stay inside these ranges and needn't reach their ends.
Inputs may be any that keep to these rules, and one draw needn't show every extreme that they name: `routes`: within each aligned block of 256 rows, no expert is named more than 64 times; some expert is named exactly 64 times in some blocks. The 2 experts of a row differ. Document numbers never fall along the positions; each document is one contiguous run.
All inputs are finite; a program needn't handle non-finite values.
Results may differ from the reference program's by a relative error of at most 0.0069.
Values may be sent and summed in bfloat16 or wider, within the bound.
A program may use at most 128 MiB of HBM per device.

```python
import math
import jax
import jax.numpy as jnp
import numpy as np
from jax import lax

D = 2048
CONV = 512
FF = 4096
TOPK = 2
TAPS = 3
TOK = 256
TOKENS = 4096
EXPERTS = 16
CAP = 64
N_SP = 16


def draw_residual(key, part):
    noise_key, column_key = jax.random.split(jax.random.fold_in(key, 11), 2)
    columns = jnp.arange(D, dtype=jnp.float32) / D
    rising = jnp.exp(jnp.log(3.0) * columns)
    scatter = jnp.exp(jax.random.uniform(column_key, (D,), jnp.float32, jnp.log(0.5), jnp.log(2.0)))
    values = jnp.clip(jax.random.normal(noise_key, (TOKENS, D), jnp.float32), -6.0, 6.0)
    return (values * rising[None, :] * scatter[None, :] * 0.6).astype(jnp.bfloat16)


def draw_mix_gain(key, part):
    columns = jnp.arange(D, dtype=jnp.float32) / D
    rising = jnp.exp(jnp.log(3.0) * (columns - 0.5))
    gain_key = jax.random.fold_in(key, 23)
    wobble = jax.random.uniform(gain_key, (D,), jnp.float32, 0.5, 1.5)
    return rising * wobble


def level_of(rng, shape, cuts, low, largest):
    factor_of, own = 1.0, jax.random.fold_in(rng, 6)
    for dim, blocks in cuts:
        draws = jnp.exp(jax.random.uniform(jax.random.fold_in(own, dim), (blocks,), jnp.float32, low / len(cuts), largest / len(cuts)))
        factor_of = factor_of * jnp.repeat(draws, shape[dim] // blocks).reshape([-1 if axis == dim else 1 for axis in range(len(shape))])
    return factor_of


def length_profile(amount, total, reach, slope):
    loads = [(1 << 20) // math.isqrt(grade ** slope) + 1 for grade in range(2, amount + 1)]
    spare, given = total - reach - (amount - 1), [1] * (amount - 1)
    while spare > 0:
        movable = [i for i in range(amount - 1) if given[i] < reach]
        whole, remaining = sum([loads[i] for i in movable]), spare
        for i in movable:
            extra = min(reach - given[i], max(1, remaining * loads[i] // whole), spare)
            given[i] = given[i] + extra
            spare = spare - extra
    return np.array([reach] + given)


def ragged_sizes(key, count, total, reach, skew):
    if count == 2:
        one = jax.random.randint(key, (), max(1, total - reach), min(reach, total - 1) + 1)
        return jnp.stack([one, total - one])
    lengths = jnp.asarray(length_profile(count, total, reach, skew), jnp.int32)
    twos = (count - 1) // 2
    giver, receiver = lengths[1:1 + 2 * twos:2], lengths[2:2 + 2 * twos:2]
    slack = jnp.minimum(giver - 1, reach - receiver)
    passed = jax.random.randint(jax.random.fold_in(key, 1), (twos,), 0, 1 << 20) % (slack + 1)
    lengths = lengths.at[1:1 + 2 * twos:2].set(giver - passed).at[2:2 + 2 * twos:2].set(receiver + passed)
    return lengths[jax.random.permutation(jax.random.fold_in(key, 2), count)]


def assign_block(stream_key, own, number, rows, count, top, limit, skew):
    sequence = jax.random.permutation(stream_key, count)
    heavy_load, ordinary = load_shares(count, rows * top, limit, skew, True), load_shares(count, rows * top, limit, skew, False)
    places = jnp.arange(count)

    def named(tallies, offset_by):
        used = int((tallies > 0).sum())
        fixed = max(1, used // 4)
        shifted = fixed + (places - fixed + offset_by * (used - fixed)) % max(1, count - fixed)
        return jnp.zeros((count,), jnp.int32).at[sequence[jnp.where(places < fixed, places, shifted)]].set(jnp.asarray(tallies, jnp.int32))

    tallies = jnp.where(number % 4 == 0, named(heavy_load, number // 4), named(ordinary, number - number // 4 - 1))
    mixed = jax.random.permutation(jax.random.fold_in(own, 3), count)
    giver, receiver = mixed[0:count // 2 * 2:2], mixed[1:count // 2 * 2:2]
    margin = jnp.minimum(tallies[giver] - 1, limit - tallies[receiver]) // 2
    margin = jnp.where((giver == sequence[0]) | (receiver == sequence[0]) | (tallies[receiver] == 0), 0, jnp.maximum(margin, 0))
    shifted = jax.random.randint(jax.random.fold_in(own, 4), (count // 2,), 0, 1 << 20) % (margin + 1)
    tallies = tallies.at[giver].add(-shifted).at[receiver].add(shifted)
    items = jnp.searchsorted(jnp.cumsum(tallies), jnp.arange(rows * top), side="right").astype(jnp.int32)
    listing = items.reshape(top, rows).T
    listing = listing[jax.random.permutation(jax.random.fold_in(own, 1), rows)]
    offset_by = jax.random.randint(jax.random.fold_in(own, 2), (rows, 1), 0, top)
    return jnp.take_along_axis(listing, (jnp.arange(top)[None, :] + offset_by) % top, axis=1)


def load_shares(number_of, total, limit, slope, full):
    weights = [(1 << 20) // math.isqrt(grade ** slope) + 1 for grade in range(1, number_of + 1)]
    largest = limit if full else min(limit, max(-(-total // number_of), total * weights[0] // sum(weights)))
    least = 1 if total - largest >= number_of - 1 else 0
    holding, spare = [largest] + [least] * (number_of - 1), total - largest - least * (number_of - 1)
    while spare > 0:
        free = [i for i in range(1, number_of) if holding[i] < largest] or [i for i in range(1, number_of) if holding[i] < limit]
        whole, left = sum([weights[i] for i in free]), spare
        for i in free:
            extra = min(limit - holding[i], max(1, left * weights[i] // whole), spare)
            holding[i] = holding[i] + extra
            spare = spare - extra
    return np.array(holding)


def centred(key, extent, scale, bound, cuts=(), kind=jnp.bfloat16):
    values = jax.random.normal(key, extent, jnp.float32) * scale
    if len(cuts) > 0:
        values = level_of(key, extent, cuts, -0.22, 0.18) * values
    return jnp.clip(values, min=-bound, max=bound).astype(kind)


def setup_inputs(seed: int = 0) -> dict:
    seeds = jax.random.split(jax.random.key(seed), 15)
    out_gate = centred(seeds[0], (TOKENS, CONV), 1.0, 6.0, ((0, 16), (1, 2)))
    in_gate = centred(seeds[1], (TOKENS, CONV), 1.0, 6.0, ((0, 16), (1, 2)))
    conv_input = centred(seeds[2], (TOKENS, CONV), 1.0, 6.0, ((0, 16), (1, 2)))
    conv_taps = centred(seeds[3], (TAPS, CONV), TAPS ** -0.5, 3.5, ((1, 2),), jnp.float32)
    out_weight = centred(seeds[4], (CONV, D), CONV ** -0.5, 0.25, ((0, 2),))
    residual = draw_residual(jax.random.fold_in(seeds[14], 71), 0)
    document = jnp.searchsorted(jnp.cumsum(ragged_sizes(seeds[6], max(2, N_SP // 4), TOKENS, 2 * TOKENS // max(2, N_SP // 4), 0)), jnp.arange(TOKENS), side="right").astype(jnp.int32)
    mix_gain = draw_mix_gain(jax.random.fold_in(seeds[14], 71), 0)
    ffn_gain = jnp.clip(1.0 + 0.18 * jax.random.normal(seeds[8], (D,), jnp.float32), 0.1, 1.9)
    routes_keys = jax.random.split(jax.random.fold_in(seeds[9], 1), TOKENS // TOK)
    routes_turns = jax.random.permutation(jax.random.fold_in(seeds[9], 3), TOKENS // TOK)
    routes = jax.vmap(lambda own, number: assign_block(jax.random.fold_in(seeds[9], 2), own, number, TOK, EXPERTS, TOPK, CAP, 1))(routes_keys, routes_turns).reshape((TOKENS, TOPK))
    route_weight = jnp.clip(0.1 + 0.9 * jax.random.uniform(seeds[10], (TOKENS, TOPK), jnp.float32) ** level_of(seeds[10], (TOKENS, TOPK), ((0, 16),), -0.2, 0.2), 0.1, 1.0)
    expert_gate = centred(seeds[11], (EXPERTS, D, FF), (D // 8) ** -0.5, 0.375, ((0, 16), (2, 2)))
    expert_up = centred(seeds[12], (EXPERTS, D, FF), (D // 8) ** -0.5, 0.375, ((0, 16), (2, 2)))
    expert_down = centred(seeds[13], (EXPERTS, FF, D), FF ** -0.5, 0.09375, ((0, 16), (2, 2)))
    return {"out_gate": out_gate, "in_gate": in_gate, "conv_input": conv_input, "conv_taps": conv_taps, "out_weight": out_weight, "residual": residual, "document": document, "mix_gain": mix_gain, "ffn_gain": ffn_gain, "routes": routes, "route_weight": route_weight, "expert_gate": expert_gate, "expert_up": expert_up, "expert_down": expert_down}


ALPHA = 8.0 ** 0.25
EPSILON = 1e-05
LIMIT = 7.0
SLOPE = 1.702

def layer_norm(stream, gain_row):
    row_mean = lax.optimization_barrier(jnp.sum(stream, axis=1)) / D
    row_spread = lax.optimization_barrier(jnp.sum(stream * stream, axis=1)) / D - row_mean * row_mean
    scaled = (stream - row_mean[:, None]) * lax.rsqrt(row_spread + EPSILON)[:, None]
    return (scaled * gain_row[None, :]).astype(jnp.bfloat16)

def clamped_unit(gate_pre, up_pre):
    gate_part = jnp.minimum(gate_pre, LIMIT)
    up_part = jnp.clip(up_pre, -LIMIT, LIMIT)
    return ((up_part + 1.0) * gate_part * jax.nn.sigmoid(SLOPE * gate_part)).astype(jnp.bfloat16)

def reference(out_gate, in_gate, conv_input, conv_taps, out_weight, residual, document, mix_gain, ffn_gain, routes, route_weight, expert_gate, expert_up, expert_down):
    product = in_gate.astype(jnp.float32) * conv_input.astype(jnp.float32)
    padded = jnp.concatenate([jnp.zeros((2, CONV), jnp.float32), product], axis=0)
    doc_marks = jnp.concatenate([jnp.full((2,), -1, jnp.int32), document.astype(jnp.int32)], axis=0)
    same_one = (doc_marks[1:-1] == document).astype(jnp.float32)[:, None]
    same_two = (doc_marks[:-2] == document).astype(jnp.float32)[:, None]
    mixed_rows = conv_taps[2][None, :] * product + same_one * conv_taps[1][None, :] * padded[1:-1] + same_two * conv_taps[0][None, :] * padded[:-2]
    conv_out = (out_gate.astype(jnp.float32) * mixed_rows).astype(jnp.bfloat16)
    mixer_sum = jnp.dot(conv_out, out_weight, preferred_element_type=jnp.float32)
    normed = layer_norm(ALPHA * residual.astype(jnp.float32) + mixer_sum, mix_gain)
    flat_routes = routes.reshape(N_SP, TOK * TOPK).astype(jnp.int32)
    one_hot = (flat_routes[:, :, None] == jnp.arange(EXPERTS, dtype=jnp.int32)[None, None, :]).astype(jnp.int32)
    rank_table = jnp.cumsum(one_hot, axis=1) - one_hot
    slot_index = lax.optimization_barrier(jnp.sum(rank_table * one_hot, axis=2)).astype(jnp.int32)
    blocks = jnp.broadcast_to(jnp.arange(N_SP, dtype=jnp.int32)[:, None], flat_routes.shape)
    source = blocks * TOK + jnp.arange(TOK * TOPK, dtype=jnp.int32)[None, :] // TOPK
    buffer = jnp.zeros((EXPERTS, N_SP, CAP, D), jnp.bfloat16).at[flat_routes, blocks, slot_index].set(normed[source])

    def one_expert(operands):
        rows_in, weight_gate, weight_up, weight_down = operands
        rows_in = rows_in.reshape(N_SP * CAP, D)
        gate_pre = jnp.dot(rows_in, weight_gate, preferred_element_type=jnp.float32)
        up_pre = jnp.dot(rows_in, weight_up, preferred_element_type=jnp.float32)
        hidden = clamped_unit(gate_pre, up_pre)
        expert_out = jnp.dot(hidden, weight_down, preferred_element_type=jnp.float32).astype(jnp.bfloat16)
        return expert_out.reshape(N_SP, CAP, D)
    results = lax.map(one_expert, (buffer, expert_gate, expert_up, expert_down))
    picked = results[flat_routes, blocks, slot_index].astype(jnp.float32).reshape(TOKENS, TOPK, D)
    ffn_out = lax.optimization_barrier(jnp.sum(picked * route_weight[:, :, None], axis=1))
    return layer_norm(ALPHA * normed.astype(jnp.float32) + ffn_out, ffn_gain)
```

```python
import functools

import jax
import jax.numpy as jnp
from jax import lax
from jax.experimental import pallas as pl
from jax.experimental.pallas import tpu as pltpu
from jax.sharding import PartitionSpec as P

ALPHA = 8.0**0.25
EPSILON = 1e-05
LIMIT = 7.0
SLOPE = 1.702
LANES = 128
HALO = 8
CHUNKS = 4
MESH = pl.DeviceIdType.MESH
F32 = jnp.float32
BF16 = jnp.bfloat16


def flipped(index, bits, count):
    total, place = 0, 1
    while place < count:
        digit = (index // place + (bits // place) % 2) % 2
        total = total + digit * place
        place *= 2
    return total


def clamped_unit(gate_pre, up_pre):
    gate_part = jnp.minimum(gate_pre, LIMIT)
    up_part = jnp.clip(up_pre, -LIMIT, LIMIT)
    return ((up_part + 1.0) * gate_part * jax.nn.sigmoid(SLOPE * gate_part)).astype(BF16)


def layer_kernel(
    n_sp,
    n_tp,
    out_gate,
    in_gate,
    conv_input,
    taps,
    out_weight,
    residual,
    marks,
    mix_gain,
    ffn_gain,
    place,
    pick,
    route_weight,
    gate_hbm,
    up_hbm,
    down_hbm,
    result,
    ext,
    ext_marks,
    halo,
    halo_marks,
    conv_all,
    weight_cols,
    stats,
    normed_all,
    xsend,
    xrecv,
    hid,
    outs,
    back,
    stream,
    w_gate,
    w_up,
    w_down,
    load_sem,
    halo_sem,
    tp_send,
    tp_recv,
    disp_send,
    disp_recv,
    x_send,
    x_recv,
    h_send,
    h_recv,
    ret_send,
    ret_recv,
):
    me = lax.axis_index("sp")
    mine = lax.axis_index("tp")
    rows, local = residual.shape
    width = local * n_tp
    slots = place.shape[0]
    cap = slots // n_sp
    group = n_sp // CHUNKS
    span = group * cap
    top = pick.shape[0]

    loads = [
        pltpu.make_async_copy(src.at[0], dst, load_sem.at[i])
        for i, (src, dst) in enumerate(((gate_hbm, w_gate), (up_hbm, w_up), (down_hbm, w_down)))
    ]
    for load in loads:
        load.start()

    def sp_peer(d):
        return {"sp": flipped(me, d, n_sp)}

    def tp_peer(p):
        return (mine + p) % n_tp

    barrier = pltpu.get_barrier_semaphore()
    for d in range(1, n_sp):
        pl.semaphore_signal(barrier, inc=1, device_id=sp_peer(d), device_id_type=MESH)
    for p in range(1, n_tp):
        pl.semaphore_signal(barrier, inc=1, device_id={"tp": tp_peer(p)}, device_id_type=MESH)
    pl.semaphore_wait(barrier, n_sp + n_tp - 2)

    def remote(src, dst, send, recv, target):
        return pltpu.make_async_remote_copy(
            src_ref=src, dst_ref=dst, send_sem=send, recv_sem=recv, device_id=target, device_id_type=MESH
        )

    def tp_copies(src_of, dst, stage):
        return [
            remote(src_of(tp_peer(p)), dst, tp_send.at[stage, p], tp_recv.at[stage, p], {"tp": tp_peer(p)})
            for p in range(1, n_tp)
        ]

    sent = []

    product = in_gate[...].astype(F32) * conv_input[...].astype(F32)
    ext[HALO:, :] = product
    ext_marks[HALO:, :] = marks[...]
    after = {"sp": (me + 1) % n_sp}
    halo_copies = [
        remote(ext.at[pl.ds(rows, HALO)], halo, halo_sem.at[0], halo_sem.at[1], after),
        remote(ext_marks.at[pl.ds(rows, HALO)], halo_marks, halo_sem.at[2], halo_sem.at[3], after),
    ]
    for copy in halo_copies:
        copy.start()
    weight_copies = tp_copies(
        lambda peer: out_weight.at[:, pl.ds(pl.multiple_of(peer * local, LANES), local)],
        weight_cols.at[mine],
        0,
    )
    for copy in weight_copies:
        copy.start()
    own_cols = pl.ds(pl.multiple_of(mine * local, LANES), local)
    weight_cols[mine] = out_weight[:, own_cols]
    for copy in halo_copies:
        copy.wait()
    ext[:HALO, :] = jnp.where(me > 0, halo[...], 0.0)
    ext_marks[:HALO, :] = halo_marks[...]
    doc = marks[...]
    same_one = (ext_marks[HALO - 1 : HALO - 1 + rows, :] == doc).astype(F32)[:, 0:1]
    same_two = (ext_marks[HALO - 2 : HALO - 2 + rows, :] == doc).astype(F32)[:, 0:1]
    mixed = (
        taps[2:3, :] * product
        + same_one * taps[1:2, :] * ext[HALO - 1 : HALO - 1 + rows, :]
        + same_two * taps[0:1, :] * ext[HALO - 2 : HALO - 2 + rows, :]
    )
    conv_all[mine] = (out_gate[...].astype(F32) * mixed).astype(BF16)
    conv_copies = tp_copies(lambda peer: conv_all.at[mine], conv_all.at[mine], 1)
    for copy in conv_copies:
        copy.start()
    stream[...] = ALPHA * residual[...].astype(F32)
    for copy in weight_copies + conv_copies:
        copy.wait_recv()
    sent += weight_copies + conv_copies
    tile_of = lambda extent: min(256, extent)
    tile = tile_of(local)

    @pl.loop(0, local // tile)
    def _(i):
        cols = pl.ds(pl.multiple_of(i * tile, tile), tile)
        total = stream[:, cols]
        for t in range(n_tp):
            total += jnp.dot(conv_all[t], weight_cols[t, :, cols], preferred_element_type=F32)
        stream[:, cols] = total

    def norm(values, gain, stage):
        sums = jnp.sum(values, axis=1, keepdims=True)
        squares = jnp.sum(values * values, axis=1, keepdims=True)
        lane = lax.broadcasted_iota(jnp.int32, (rows, LANES), 1)
        stats[stage - 2, mine] = jnp.where(lane < LANES // 2, sums, squares)
        copies = tp_copies(lambda peer: stats.at[stage - 2, mine], stats.at[stage - 2, mine], stage)
        for copy in copies:
            copy.start()
        for copy in copies:
            copy.wait()
        both = stats[stage - 2, 0]
        for t in range(1, n_tp):
            both = both + stats[stage - 2, t]
        mean = both[:, 0:1] / width
        spread = both[:, LANES // 2 : LANES // 2 + 1] / width - mean * mean
        return ((values - mean) * lax.rsqrt(spread + EPSILON) * gain[...]).astype(BF16)

    normed_all[mine] = norm(stream[...], mix_gain, 2)
    normed_copies = tp_copies(lambda peer: normed_all.at[mine], normed_all.at[mine], 4)
    for copy in normed_copies:
        copy.start()
    sent += normed_copies

    def placed(t):
        @pl.loop(0, slots // 256)
        def _(i):
            band = pl.ds(pl.multiple_of(i * 256, 256), 256)
            xsend[t, band, :] = jnp.dot(place[band, :], normed_all[t], preferred_element_type=F32).astype(BF16)

    far = range(CHUNKS // 2, CHUNKS)
    dispatch = {}

    def send_rows(j):
        for d in range(max(1, j * group), (j + 1) * group):
            band = pl.ds(d * cap, cap)
            if j in far:
                src, dst = xsend.at[mine, band], xrecv.at[mine, band]
            else:
                src, dst = xsend.at[:, band], xrecv.at[:, band]
            dispatch[d] = remote(src, dst, disp_send.at[d], disp_recv.at[d], sp_peer(d))
            dispatch[d].start()

    placed(mine)
    for j in far:
        send_rows(j)
    for copy in normed_copies:
        copy.wait_recv()
    for p in range(1, n_tp):
        placed(tp_peer(p))
    for j in range(CHUNKS // 2):
        send_rows(j)
    for t in range(n_tp):
        xrecv[t, 0:cap, :] = xsend[t, 0:cap, :]
    for load in loads:
        load.wait()

    x_copies, h_copies, returns = {}, {}, []

    def share_rows(j):
        for d in range(j * group, (j + 1) * group):
            dispatch[d].wait_recv()
        band = pl.ds(j * span, span)
        x_copies[j] = [
            remote(
                xrecv.at[mine, band], xrecv.at[mine, band], x_send.at[j, p], x_recv.at[j, p], {"tp": tp_peer(p)}
            )
            for p in range(1, n_tp)
        ]
        for copy in x_copies[j]:
            copy.start()

    def hidden_of(j):
        if j in far:
            for copy in x_copies[j]:
                copy.wait_recv()
        else:
            for d in range(max(1, j * group), (j + 1) * group):
                dispatch[d].wait_recv()
        band = slice(j * span, (j + 1) * span)
        units = w_gate.shape[1]
        step = tile_of(units)

        @pl.loop(0, units // step)
        def _(i):
            cols = pl.ds(pl.multiple_of(i * step, step), step)
            gate_pre = jnp.zeros((span, step), F32)
            up_pre = jnp.zeros((span, step), F32)
            for t in range(n_tp):
                x = xrecv[t, band, :]
                gate_pre += jnp.dot(x, w_gate[t * local : (t + 1) * local, cols], preferred_element_type=F32)
                up_pre += jnp.dot(x, w_up[t * local : (t + 1) * local, cols], preferred_element_type=F32)
            hid[mine, band, cols] = clamped_unit(gate_pre, up_pre)

        where = pl.ds(j * span, span)
        h_copies[j] = [
            remote(hid.at[mine, where], hid.at[mine, where], h_send.at[j, p], h_recv.at[j, p], {"tp": tp_peer(p)})
            for p in range(1, n_tp)
        ]
        for copy in h_copies[j]:
            copy.start()

    def down_of(j):
        for copy in h_copies[j]:
            copy.wait_recv()
        band = slice(j * span, (j + 1) * span)
        units = w_gate.shape[1]

        @pl.loop(0, local // tile)
        def _(i):
            cols = pl.ds(pl.multiple_of(i * tile, tile), tile)
            total = jnp.zeros((span, tile), F32)
            for t in range(n_tp):
                total += jnp.dot(hid[t, band, :], w_down[t * units : (t + 1) * units, cols], preferred_element_type=F32)
            outs[band, cols] = total.astype(BF16)

        for d in range(max(1, j * group), (j + 1) * group):
            where = pl.ds(d * cap, cap)
            copy = remote(outs.at[where], back.at[where], ret_send.at[d], ret_recv.at[d], sp_peer(d))
            copy.start()
            returns.append(copy)

    hidden_of(0)
    for j in far:
        share_rows(j)
    down_of(0)
    for j in far:
        hidden_of(j)
    for j in range(1, CHUNKS // 2):
        hidden_of(j)
    for j in far:
        down_of(j)
    for j in range(1, CHUNKS // 2):
        down_of(j)
    back[0:cap, :] = outs[0:cap, :]
    for copy in returns:
        copy.wait_recv()

    @pl.loop(0, local // tile)
    def _(i):
        cols = pl.ds(pl.multiple_of(i * tile, tile), tile)
        total = jnp.zeros((rows, tile), F32)
        for k in range(top):
            picked = jnp.dot(pick[k], back[:, cols], preferred_element_type=F32)
            total += picked * route_weight[:, k : k + 1]
        stream[:, cols] = ALPHA * normed_all[mine, :, cols].astype(F32) + total

    result[...] = norm(stream[...], ffn_gain, 3)
    for copy in sent + returns:
        copy.wait_send()
    for d in dispatch:
        dispatch[d].wait_send()
    for table in (x_copies, h_copies):
        for j in table:
            for copy in table[j]:
                copy.wait_send()


def per_device(
    out_gate,
    in_gate,
    conv_input,
    conv_taps,
    out_weight,
    residual,
    document,
    mix_gain,
    ffn_gain,
    routes,
    route_weight,
    expert_gate,
    expert_up,
    expert_down,
):
    n_sp, n_tp = lax.axis_size("sp"), lax.axis_size("tp")
    rows, local = residual.shape
    channels = out_gate.shape[1]
    top = routes.shape[1]
    cap = 2 * rows * top // n_sp
    slots = n_sp * cap
    units = expert_gate.shape[2]

    flat_routes = routes.reshape(-1)
    experts = jnp.arange(n_sp, dtype=jnp.int32)
    one_hot = (flat_routes[:, None] == experts[None, :]).astype(jnp.int32)
    rank_table = jnp.cumsum(one_hot, axis=0) - one_hot
    slot_index = jnp.sum(rank_table * one_hot, axis=1)
    relative = jnp.bitwise_xor(flat_routes, lax.axis_index("sp").astype(jnp.int32))
    target = (relative * cap + slot_index).reshape(rows, top)
    slot_ids = jnp.arange(slots, dtype=jnp.int32)
    pick = (target.T[:, :, None] == slot_ids[None, None, :]).astype(BF16)
    place = jnp.any(slot_ids[:, None, None] == target.T[None, :, :], axis=1).astype(BF16)
    marks = jnp.broadcast_to(document.astype(F32)[:, None], (rows, LANES))

    vmem = pl.BlockSpec(memory_space=pltpu.VMEM)
    hbm = pl.BlockSpec(memory_space=pl.ANY)
    dma = pltpu.SemaphoreType.DMA
    return pl.pallas_call(
        functools.partial(layer_kernel, n_sp, n_tp),
        out_shape=jax.ShapeDtypeStruct((rows, local), BF16),
        in_specs=[vmem] * 12 + [hbm] * 3,
        out_specs=vmem,
        scratch_shapes=[
            pltpu.VMEM((rows + HALO, channels), F32),
            pltpu.VMEM((rows + HALO, LANES), F32),
            pltpu.VMEM((HALO, channels), F32),
            pltpu.VMEM((HALO, LANES), F32),
            pltpu.VMEM((n_tp, rows, channels), BF16),
            pltpu.VMEM((n_tp, channels, local), BF16),
            pltpu.VMEM((2, n_tp, rows, LANES), F32),
            pltpu.VMEM((n_tp, rows, local), BF16),
            pltpu.VMEM((n_tp, slots, local), BF16),
            pltpu.VMEM((n_tp, slots, local), BF16),
            pltpu.VMEM((n_tp, slots, units), BF16),
            pltpu.VMEM((slots, local), BF16),
            pltpu.VMEM((slots, local), BF16),
            pltpu.VMEM((rows, local), F32),
            pltpu.VMEM(expert_gate.shape[1:], BF16),
            pltpu.VMEM(expert_up.shape[1:], BF16),
            pltpu.VMEM(expert_down.shape[1:], BF16),
            dma((3,)),
            dma((4,)),
            dma((5, n_tp)),
            dma((5, n_tp)),
            dma((n_sp,)),
            dma((n_sp,)),
            dma((CHUNKS, n_tp)),
            dma((CHUNKS, n_tp)),
            dma((CHUNKS, n_tp)),
            dma((CHUNKS, n_tp)),
            dma((n_sp,)),
            dma((n_sp,)),
        ],
        compiler_params=pltpu.CompilerParams(
            collective_id=0, has_side_effects=True, vmem_limit_bytes=67043328
        ),
    )(
        out_gate,
        in_gate,
        conv_input,
        conv_taps,
        out_weight,
        residual,
        marks,
        mix_gain[None, :],
        ffn_gain[None, :],
        place,
        pick,
        route_weight,
        expert_gate,
        expert_up,
        expert_down,
    )


def solution(mesh):
    placed = (
        P("sp", "tp"),
        P("sp", "tp"),
        P("sp", "tp"),
        P(None, "tp"),
        P("tp", None),
        P("sp", "tp"),
        P("sp"),
        P("tp"),
        P("tp"),
        P("sp", None),
        P("sp", None),
        P("sp", None, "tp"),
        P("sp", None, "tp"),
        P("sp", None, "tp"),
    )
    return jax.shard_map(
        per_device, mesh=mesh, in_specs=placed, out_specs=P("sp", "tp"), check_vma=False
    )
```

```python
import functools

import jax
import jax.numpy as jnp
from jax import lax
from jax.experimental import pallas as pl
from jax.experimental.pallas import tpu as pltpu
from jax.sharding import PartitionSpec as P

ALPHA = 8.0**0.25
EPSILON = 1e-05
LIMIT = 7.0
SLOPE = 1.702
LANES = 128
HALO = 8
CHUNKS = 8
MESH = pl.DeviceIdType.MESH
F32 = jnp.float32
BF16 = jnp.bfloat16


def flipped(index, bits, count):
    total, place = 0, 1
    while place < count:
        digit = (index // place + (bits // place) % 2) % 2
        total = total + digit * place
        place *= 2
    return total


def clamped_unit(gate_pre, up_pre):
    gate_part = jnp.minimum(gate_pre, LIMIT)
    up_part = jnp.clip(up_pre, -LIMIT, LIMIT)
    return ((up_part + 1.0) * gate_part * jax.nn.sigmoid(SLOPE * gate_part)).astype(BF16)


def layer_kernel(
    n_sp,
    n_tp,
    out_gate,
    in_gate,
    conv_input,
    taps,
    out_weight,
    residual,
    document,
    mix_gain,
    ffn_gain,
    routes,
    route_weight,
    gate_hbm,
    up_hbm,
    down_hbm,
    result,
    place,
    pick,
    marks,
    shares,
    ext,
    ext_marks,
    halo,
    halo_marks,
    conv_all,
    weight_cols,
    stats,
    normed_all,
    xsend,
    xrecv,
    hid,
    outs,
    back,
    stream,
    w_gate,
    w_up,
    w_down,
    load_sem,
    halo_sem,
    tp_send,
    tp_recv,
    disp_send,
    disp_recv,
    x_send,
    x_recv,
    h_send,
    h_recv,
    ret_send,
    ret_recv,
):
    me = lax.axis_index("sp")
    mine = lax.axis_index("tp")
    rows, local = residual.shape
    width = local * n_tp
    top = routes.shape[0]
    cap = 2 * rows * top // n_sp
    slots = n_sp * cap
    group = n_sp // CHUNKS
    span = group * cap

    loads = [
        pltpu.make_async_copy(src.at[0], dst, load_sem.at[i])
        for i, (src, dst) in enumerate(((gate_hbm, w_gate), (up_hbm, w_up), (down_hbm, w_down)))
    ]
    for load in loads:
        load.start()

    def sp_peer(d):
        return {"sp": flipped(me, d, n_sp)}

    def tp_peer(p):
        return (mine + p) % n_tp

    barrier = pltpu.get_barrier_semaphore()
    for d in range(1, n_sp):
        pl.semaphore_signal(barrier, inc=1, device_id=sp_peer(d), device_id_type=MESH)
    for p in range(1, n_tp):
        pl.semaphore_signal(barrier, inc=1, device_id={"tp": tp_peer(p)}, device_id_type=MESH)
    pl.semaphore_wait(barrier, n_sp + n_tp - 2)

    def remote(src, dst, send, recv, target):
        return pltpu.make_async_remote_copy(
            src_ref=src, dst_ref=dst, send_sem=send, recv_sem=recv, device_id=target, device_id_type=MESH
        )

    def tp_copies(src_of, dst, stage):
        return [
            remote(src_of(tp_peer(p)), dst, tp_send.at[stage, p], tp_recv.at[stage, p], {"tp": tp_peer(p)})
            for p in range(1, n_tp)
        ]

    sent = []

    def column(row):
        return jnp.transpose(jnp.broadcast_to(row.astype(F32), (LANES, rows)))


    product = in_gate[...].astype(F32) * conv_input[...].astype(F32)
    ext[HALO:, :] = product
    marks[...] = column(document[...])
    ext_marks[HALO:, :] = marks[...]
    after = {"sp": (me + 1) % n_sp}
    halo_copies = [
        remote(ext.at[pl.ds(rows, HALO)], halo, halo_sem.at[0], halo_sem.at[1], after),
        remote(ext_marks.at[pl.ds(rows, HALO)], halo_marks, halo_sem.at[2], halo_sem.at[3], after),
    ]
    for copy in halo_copies:
        copy.start()
    weight_copies = tp_copies(
        lambda peer: out_weight.at[:, pl.ds(pl.multiple_of(peer * local, LANES), local)],
        weight_cols.at[mine],
        0,
    )
    for copy in weight_copies:
        copy.start()
    own_cols = pl.ds(pl.multiple_of(mine * local, LANES), local)
    weight_cols[mine] = out_weight[:, own_cols]
    for copy in halo_copies:
        copy.wait()
    ext[:HALO, :] = jnp.where(me > 0, halo[...], 0.0)
    ext_marks[:HALO, :] = halo_marks[...]
    doc = marks[...]
    same_one = (ext_marks[HALO - 1 : HALO - 1 + rows, :] == doc).astype(F32)[:, 0:1]
    same_two = (ext_marks[HALO - 2 : HALO - 2 + rows, :] == doc).astype(F32)[:, 0:1]
    mixed = (
        taps[2:3, :] * product
        + same_one * taps[1:2, :] * ext[HALO - 1 : HALO - 1 + rows, :]
        + same_two * taps[0:1, :] * ext[HALO - 2 : HALO - 2 + rows, :]
    )
    conv_all[mine] = (out_gate[...].astype(F32) * mixed).astype(BF16)
    conv_copies = tp_copies(lambda peer: conv_all.at[mine], conv_all.at[mine], 1)
    for copy in conv_copies:
        copy.start()
    stream[...] = ALPHA * residual[...].astype(F32)

    lane = lax.broadcasted_iota(jnp.int32, (rows, LANES), 1).astype(F32)
    named = [column(routes[k : k + 1, :]) for k in range(top)]
    one_hot = [jnp.where(named[k] == lane, 1.0, 0.0) for k in range(top)]
    taken = one_hot[0]
    for k in range(1, top):
        taken = taken + one_hot[k]
    earlier = lax.broadcasted_iota(jnp.int32, (rows, rows), 1) < lax.broadcasted_iota(jnp.int32, (rows, rows), 0)
    rank = jnp.dot(jnp.where(earlier, 1.0, 0.0).astype(BF16), taken.astype(BF16), preferred_element_type=F32)
    slot_lane = lax.broadcasted_iota(jnp.int32, (rows, slots), 1)
    slot_row = lax.broadcasted_iota(jnp.int32, (slots, rows), 0)
    filled = None
    for k in range(top):
        within = jnp.sum(rank * one_hot[k], axis=1, keepdims=True)
        relative = jnp.bitwise_xor(named[k].astype(jnp.int32), me)
        slot = relative * cap + within.astype(jnp.int32)
        pick[k] = jnp.where(slot_lane == slot[:, 0:1], 1.0, 0.0).astype(BF16)
        across = jnp.transpose(slot.astype(F32))[0:1, :].astype(jnp.int32)
        hit = jnp.where(slot_row == across, 1.0, 0.0)
        filled = hit if filled is None else filled + hit
        shares[k] = column(route_weight[k : k + 1, :])
    place[...] = filled.astype(BF16)
    for copy in weight_copies + conv_copies:
        copy.wait_recv()
    sent += weight_copies + conv_copies
    tile_of = lambda extent: min(256, extent)
    tile = tile_of(local)

    @pl.loop(0, local // tile)
    def _(i):
        cols = pl.ds(pl.multiple_of(i * tile, tile), tile)
        total = stream[:, cols]
        for t in range(n_tp):
            total += jnp.dot(conv_all[t], weight_cols[t, :, cols], preferred_element_type=F32)
        stream[:, cols] = total

    def norm(values, gain, stage):
        sums = jnp.sum(values, axis=1, keepdims=True)
        squares = jnp.sum(values * values, axis=1, keepdims=True)
        lane = lax.broadcasted_iota(jnp.int32, (rows, LANES), 1)
        stats[stage - 2, mine] = jnp.where(lane < LANES // 2, sums, squares)
        copies = tp_copies(lambda peer: stats.at[stage - 2, mine], stats.at[stage - 2, mine], stage)
        for copy in copies:
            copy.start()
        for copy in copies:
            copy.wait()
        both = stats[stage - 2, 0]
        for t in range(1, n_tp):
            both = both + stats[stage - 2, t]
        mean = both[:, 0:1] / width
        spread = both[:, LANES // 2 : LANES // 2 + 1] / width - mean * mean
        return ((values - mean) * lax.rsqrt(spread + EPSILON) * gain[...]).astype(BF16)

    normed_all[mine] = norm(stream[...], mix_gain, 2)
    normed_copies = tp_copies(lambda peer: normed_all.at[mine], normed_all.at[mine], 4)
    for copy in normed_copies:
        copy.start()
    sent += normed_copies

    def placed(t):
        @pl.loop(0, slots // 256)
        def _(i):
            band = pl.ds(pl.multiple_of(i * 256, 256), 256)
            xsend[t, band, :] = jnp.dot(place[band, :], normed_all[t], preferred_element_type=F32).astype(BF16)

    far = (6, 7)
    dispatch = {}

    def send_rows(j):
        for d in range(max(1, j * group), (j + 1) * group):
            band = pl.ds(d * cap, cap)
            if j in far:
                src, dst = xsend.at[mine, band], xrecv.at[mine, band]
            else:
                src, dst = xsend.at[:, band], xrecv.at[:, band]
            dispatch[d] = remote(src, dst, disp_send.at[d], disp_recv.at[d], sp_peer(d))
            dispatch[d].start()

    placed(mine)
    for j in far:
        send_rows(j)
    for copy in normed_copies:
        copy.wait_recv()
    for p in range(1, n_tp):
        placed(tp_peer(p))
    for j in (0, 1, 4, 5, 2, 3):
        send_rows(j)
    for t in range(n_tp):
        xrecv[t, 0:cap, :] = xsend[t, 0:cap, :]
    for load in loads:
        load.wait()

    x_copies, h_copies, returns = {}, {}, []

    def share_rows(j):
        for d in range(j * group, (j + 1) * group):
            dispatch[d].wait_recv()
        band = pl.ds(j * span, span)
        x_copies[j] = [
            remote(
                xrecv.at[mine, band], xrecv.at[mine, band], x_send.at[j, p], x_recv.at[j, p], {"tp": tp_peer(p)}
            )
            for p in range(1, n_tp)
        ]
        for copy in x_copies[j]:
            copy.start()

    def hidden_of(j):
        if j in far:
            for copy in x_copies[j]:
                copy.wait_recv()
        else:
            for d in range(max(1, j * group), (j + 1) * group):
                dispatch[d].wait_recv()
        band = slice(j * span, (j + 1) * span)
        units = w_gate.shape[1]
        step = tile_of(units)

        @pl.loop(0, units // step)
        def _(i):
            cols = pl.ds(pl.multiple_of(i * step, step), step)
            gate_pre = jnp.zeros((span, step), F32)
            up_pre = jnp.zeros((span, step), F32)
            for t in range(n_tp):
                x = xrecv[t, band, :]
                gate_pre += jnp.dot(x, w_gate[t * local : (t + 1) * local, cols], preferred_element_type=F32)
                up_pre += jnp.dot(x, w_up[t * local : (t + 1) * local, cols], preferred_element_type=F32)
            hid[mine, band, cols] = clamped_unit(gate_pre, up_pre)

        where = pl.ds(j * span, span)
        h_copies[j] = [
            remote(hid.at[mine, where], hid.at[mine, where], h_send.at[j, p], h_recv.at[j, p], {"tp": tp_peer(p)})
            for p in range(1, n_tp)
        ]
        for copy in h_copies[j]:
            copy.start()

    def down_of(j):
        for copy in h_copies[j]:
            copy.wait_recv()
        band = slice(j * span, (j + 1) * span)
        units = w_gate.shape[1]

        @pl.loop(0, local // tile)
        def _(i):
            cols = pl.ds(pl.multiple_of(i * tile, tile), tile)
            total = jnp.zeros((span, tile), F32)
            for t in range(n_tp):
                total += jnp.dot(hid[t, band, :], w_down[t * units : (t + 1) * units, cols], preferred_element_type=F32)
            outs[band, cols] = total.astype(BF16)

        for d in range(max(1, j * group), (j + 1) * group):
            where = pl.ds(d * cap, cap)
            copy = remote(outs.at[where], back.at[where], ret_send.at[d], ret_recv.at[d], sp_peer(d))
            copy.start()
            returns.append(copy)

    hidden_of(0)
    hidden_of(1)
    share_rows(6)
    share_rows(7)
    hidden_of(4)
    down_of(0)
    down_of(1)
    hidden_of(5)
    hidden_of(6)
    down_of(4)
    hidden_of(7)
    down_of(5)
    hidden_of(2)
    down_of(6)
    hidden_of(3)
    down_of(7)
    down_of(2)
    down_of(3)
    back[0:cap, :] = outs[0:cap, :]
    for copy in returns:
        copy.wait_recv()

    @pl.loop(0, local // tile)
    def _(i):
        cols = pl.ds(pl.multiple_of(i * tile, tile), tile)
        total = jnp.zeros((rows, tile), F32)
        for k in range(top):
            picked = jnp.dot(pick[k], back[:, cols], preferred_element_type=F32)
            total += picked * shares[k][:, 0:1]
        stream[:, cols] = ALPHA * normed_all[mine, :, cols].astype(F32) + total

    result[...] = norm(stream[...], ffn_gain, 3)
    for copy in sent + returns:
        copy.wait_send()
    for d in dispatch:
        dispatch[d].wait_send()
    for table in (x_copies, h_copies):
        for j in table:
            for copy in table[j]:
                copy.wait_send()


def per_device(
    out_gate,
    in_gate,
    conv_input,
    conv_taps,
    out_weight,
    residual,
    document,
    mix_gain,
    ffn_gain,
    routes,
    route_weight,
    expert_gate,
    expert_up,
    expert_down,
):
    n_sp, n_tp = lax.axis_size("sp"), lax.axis_size("tp")
    rows, local = residual.shape
    channels = out_gate.shape[1]
    top = routes.shape[1]
    cap = 2 * rows * top // n_sp
    slots = n_sp * cap
    units = expert_gate.shape[2]

    vmem = pl.BlockSpec(memory_space=pltpu.VMEM)
    hbm = pl.BlockSpec(memory_space=pl.ANY)
    dma = pltpu.SemaphoreType.DMA
    return pl.pallas_call(
        functools.partial(layer_kernel, n_sp, n_tp),
        out_shape=jax.ShapeDtypeStruct((rows, local), BF16),
        in_specs=[vmem] * 11 + [hbm] * 3,
        out_specs=vmem,
        scratch_shapes=[
            pltpu.VMEM((slots, rows), BF16),
            pltpu.VMEM((top, rows, slots), BF16),
            pltpu.VMEM((rows, LANES), F32),
            pltpu.VMEM((top, rows, LANES), F32),
            pltpu.VMEM((rows + HALO, channels), F32),
            pltpu.VMEM((rows + HALO, LANES), F32),
            pltpu.VMEM((HALO, channels), F32),
            pltpu.VMEM((HALO, LANES), F32),
            pltpu.VMEM((n_tp, rows, channels), BF16),
            pltpu.VMEM((n_tp, channels, local), BF16),
            pltpu.VMEM((2, n_tp, rows, LANES), F32),
            pltpu.VMEM((n_tp, rows, local), BF16),
            pltpu.VMEM((n_tp, slots, local), BF16),
            pltpu.VMEM((n_tp, slots, local), BF16),
            pltpu.VMEM((n_tp, slots, units), BF16),
            pltpu.VMEM((slots, local), BF16),
            pltpu.VMEM((slots, local), BF16),
            pltpu.VMEM((rows, local), F32),
            pltpu.VMEM(expert_gate.shape[1:], BF16),
            pltpu.VMEM(expert_up.shape[1:], BF16),
            pltpu.VMEM(expert_down.shape[1:], BF16),
            dma((3,)),
            dma((4,)),
            dma((5, n_tp)),
            dma((5, n_tp)),
            dma((n_sp,)),
            dma((n_sp,)),
            dma((CHUNKS, n_tp)),
            dma((CHUNKS, n_tp)),
            dma((CHUNKS, n_tp)),
            dma((CHUNKS, n_tp)),
            dma((n_sp,)),
            dma((n_sp,)),
        ],
        compiler_params=pltpu.CompilerParams(
            collective_id=0, has_side_effects=True, vmem_limit_bytes=67043328
        ),
    )(
        out_gate,
        in_gate,
        conv_input,
        conv_taps,
        out_weight,
        residual,
        document[None, :],
        mix_gain[None, :],
        ffn_gain[None, :],
        routes.T,
        route_weight.T,
        expert_gate,
        expert_up,
        expert_down,
    )


def solution(mesh):
    placed = (
        P("sp", "tp"),
        P("sp", "tp"),
        P("sp", "tp"),
        P(None, "tp"),
        P("tp", None),
        P("sp", "tp"),
        P("sp"),
        P("tp"),
        P("tp"),
        P("sp", None),
        P("sp", None),
        P("sp", None, "tp"),
        P("sp", None, "tp"),
        P("sp", None, "tp"),
    )
    return jax.shard_map(
        per_device, mesh=mesh, in_specs=placed, out_specs=P("sp", "tp"), check_vma=False
    )
```
